32 devices in a mesh: sp: 16 (over z, x, core), tp: 2 (over y).
Axes of the slice: x: 2, y: 2, z: 4, core: 2. Of those that a mesh axis runs over, the one named last changes fastest.
Arguments:
- queries: bfloat16 [10240, 1024], P('sp', 'tp'), may hold values from -160 to 160
- keys: bfloat16 [10240, 256], P('sp', 'tp'), may hold values from -24 to 24
- values: bfloat16 [10240, 256], P('sp', 'tp'), may hold values from -6 to 6
- documents: int32 [10240], P('sp'), may hold values from 0 to 3, never falling along the last dimension, each value on 1 to 5120 neighbouring positions
- sinks: float32 [16], P('tp'), may hold values from -1 to 4
- out_weight: bfloat16 [1024, 2048], replicated, may hold values from -0.1875 to 0.1875
- residual: bfloat16 [10240, 2048], P(('sp', 'tp')), may hold values from -3 to 3
- norm_gain: float32 [2048], replicated, may hold values from 0.1 to 1.9
- up_weight: bfloat16 [2048, 8192], P('sp', 'tp'), may hold values from -0.125 to 0.125
- down_weight: bfloat16 [8192, 2048], P('tp', 'sp'), may hold values from -0.0625 to 0.0625
Outputs:
- layer_out: bfloat16 [10240, 2048], P(('sp', 'tp'))
The draws below stay inside these ranges and needn't reach their ends.
Inputs may be any that keep to these rules, and one draw needn't show every extreme that they name: `documents`: document numbers never fall along the positions; each document holds at most 5120 positions.
All inputs are finite; a program needn't handle non-finite values.
Results may differ from the reference program's by a relative error of at most 0.0095.
Values may be sent and summed in bfloat16 or wider, within the bound.
No kernel may reach another device: no remote copies, remote signals or barrier semaphores. Data moves between devices by JAX's collectives and lax.ppermute only.
A program may use at most 128 MiB of HBM per device.

```python
import math
import jax
import jax.numpy as jnp
import numpy as np
from jax import lax

D = 2048
QUERY_HEADS = 16
KEY_VALUE_HEADS = 4
HEAD_SIZE = 64
FF = 8192
WINDOW_REACH = 128
TOK_DEV = 640
PACK_TOKENS = 10240
ATTN = 1024
FF_DEV = 4096
DOCS = 4
N_SP = 16
N_TP = 2


def drawn(key):
    starting_keys = jax.random.normal(jax.random.fold_in(key, 11), (PACK_TOKENS, KEY_VALUE_HEADS, HEAD_SIZE), jnp.float32)
    base_queries = jax.random.normal(jax.random.fold_in(key, 12), (PACK_TOKENS, QUERY_HEADS, HEAD_SIZE), jnp.float32)
    output_keys = starting_keys
    output_queries = base_queries
    return (output_queries.reshape(PACK_TOKENS, QUERY_HEADS * HEAD_SIZE).astype(jnp.bfloat16), output_keys.reshape(PACK_TOKENS, KEY_VALUE_HEADS * HEAD_SIZE).astype(jnp.bfloat16))


def draw_queries(key, part):
    return drawn(key)[0]


def draw_keys(key, part):
    return drawn(key)[1]


def shard_levels(stream_key, dims, cuts, low, largest):
    level = 1.0
    for dim, blocks in cuts:
        heights = jax.random.uniform(jax.random.fold_in(jax.random.fold_in(stream_key, 6), dim), (blocks,), jnp.float32, low / len(cuts), largest / len(cuts))
        level = level * jnp.repeat(jnp.exp(heights), dims[dim] // blocks).reshape((-1,) + (1,) * (len(dims) - 1 - dim))
    return level


def split_up(count, total, limit, lean):
    loads = [(1 << 20) // math.isqrt(grade ** lean) + 1 for grade in range(2, count + 1)]
    surplus, counts = total - limit - (count - 1), [1] * (count - 1)
    while surplus > 0:
        free = [i for i in range(count - 1) if counts[i] < limit]
        mass, budget = sum([loads[i] for i in free]), surplus
        for i in free:
            more = min(limit - counts[i], max(1, budget * loads[i] // mass), surplus)
            counts[i] = counts[i] + more
            surplus = surplus - more
    return np.array([limit] + counts)


def ragged(rng, amount, total, limit, lean):
    if amount == 2:
        one = jax.random.randint(rng, (), max(1, total - limit), min(limit, total - 1) + 1)
        return jnp.stack([one, total - one])
    lengths = jnp.asarray(split_up(amount, total, limit, lean), jnp.int32)
    couples = (amount - 1) // 2
    giver, taker = lengths[1:1 + 2 * couples:2], lengths[2:2 + 2 * couples:2]
    margin = jnp.minimum(giver - 1, limit - taker)
    shifted = jax.random.randint(jax.random.fold_in(rng, 1), (couples,), 0, 1 << 20) % (margin + 1)
    lengths = lengths.at[1:1 + 2 * couples:2].set(giver - shifted).at[2:2 + 2 * couples:2].set(taker + shifted)
    return lengths[jax.random.permutation(jax.random.fold_in(rng, 2), amount)]


def noise(own_key, shape, spread, bound, pieces=(), kind=jnp.bfloat16):
    array = jax.random.normal(own_key, shape, jnp.float32) * spread
    if len(pieces) > 0:
        array = shard_levels(own_key, shape, pieces, -0.22, 0.18) * array
    return jnp.clip(array, min=-bound, max=bound).astype(kind)


def setup_inputs(seed: int = 0) -> dict:
    streams_of = jax.random.split(jax.random.key(seed), 11)
    queries = draw_queries(jax.random.fold_in(streams_of[10], 71), 0)
    keys = draw_keys(jax.random.fold_in(streams_of[10], 71), 0)
    values = noise(streams_of[2], (PACK_TOKENS, KEY_VALUE_HEADS * HEAD_SIZE), 1.0, 6.0, ((0, 16), (1, 2)))
    documents = jnp.searchsorted(jnp.cumsum(ragged(streams_of[3], DOCS, PACK_TOKENS, 8 * TOK_DEV, 1)), jnp.arange(PACK_TOKENS), side="right").astype(jnp.int32)
    sinks = jnp.clip(-1.0 + 5.0 * jax.random.uniform(streams_of[4], (QUERY_HEADS,), jnp.float32) ** shard_levels(streams_of[4], (QUERY_HEADS,), ((0, 2),), -0.2, 0.2), -1.0, 4.0)
    out_weight = noise(streams_of[5], (ATTN, D), ATTN ** -0.5, 0.1875)
    residual = noise(streams_of[6], (PACK_TOKENS, D), 0.5, 3.0, ((0, 32),))
    norm_gain = jnp.clip(1.0 + 0.18 * jax.random.normal(streams_of[7], (D,), jnp.float32), 0.1, 1.9)
    up_weight = noise(streams_of[8], (D, FF), D ** -0.5, 0.125, ((0, 16), (1, 2)))
    down_weight = noise(streams_of[9], (FF, D), FF ** -0.5, 0.0625, ((0, 2), (1, 16)))
    return {"queries": queries, "keys": keys, "values": values, "documents": documents, "sinks": sinks, "out_weight": out_weight, "residual": residual, "norm_gain": norm_gain, "up_weight": up_weight, "down_weight": down_weight}


masked_score = -1e+30
epsilon = 1e-06

def rounded(value):
    return lax.optimization_barrier(value.astype(jnp.bfloat16))

def reference(queries, keys, values, documents, sinks, out_weight, residual, norm_gain, up_weight, down_weight):
    query_group = QUERY_HEADS // KEY_VALUE_HEADS
    block_list = PACK_TOKENS // WINDOW_REACH
    key_matrix = jnp.concatenate([jnp.zeros((WINDOW_REACH, KEY_VALUE_HEADS * HEAD_SIZE), jnp.bfloat16), keys], axis=0).reshape(block_list + 1, WINDOW_REACH, KEY_VALUE_HEADS, HEAD_SIZE)
    value_matrix = jnp.concatenate([jnp.zeros((WINDOW_REACH, KEY_VALUE_HEADS * HEAD_SIZE), jnp.bfloat16), values], axis=0).reshape(block_list + 1, WINDOW_REACH, KEY_VALUE_HEADS, HEAD_SIZE)
    doc_ids = documents.astype(jnp.int32)
    key_docs = jnp.concatenate([jnp.full((WINDOW_REACH,), -1, jnp.int32), doc_ids], axis=0).reshape(block_list + 1, WINDOW_REACH)
    query_docs = doc_ids.reshape(block_list, WINDOW_REACH)
    grouped_queries = queries.reshape(block_list, WINDOW_REACH, KEY_VALUE_HEADS, query_group, HEAD_SIZE)
    head_sink_logit = sinks.astype(jnp.float32).reshape(KEY_VALUE_HEADS, query_group, 1)
    row_index = jnp.arange(WINDOW_REACH, dtype=jnp.int32)[:, None]
    col_index = jnp.arange(2 * WINDOW_REACH, dtype=jnp.int32)[None, :]
    distance = WINDOW_REACH + row_index - col_index
    near = (distance >= 0) & (distance < WINDOW_REACH)

    def one_block(items):
        block_queries, early_keys, late_keys, early_values, late_values, early_docs, late_docs, own_docs = items
        band_keys = jnp.concatenate([early_keys, late_keys], axis=0).astype(jnp.float32)
        band_values = jnp.concatenate([early_values, late_values], axis=0).astype(jnp.float32)
        band_docs = jnp.concatenate([early_docs, late_docs], axis=0)
        visible = (near & (band_docs[None, :] == own_docs[:, None]))[None, None]
        scores = jnp.einsum('qhgd,shd->hgqs', block_queries.astype(jnp.float32), band_keys) * HEAD_SIZE ** (-0.5)
        scores = jnp.where(visible, scores, masked_score)
        top = jnp.maximum(lax.optimization_barrier(jnp.max(scores, axis=-1)), head_sink_logit)
        exponent = jnp.where(visible, jnp.exp(scores - top[..., None]), 0.0)
        total = jnp.exp(head_sink_logit - top) + lax.optimization_barrier(jnp.sum(exponent, axis=-1))
        shares = rounded(exponent / total[..., None])
        attended = jnp.einsum('hgqs,shd->qhgd', shares.astype(jnp.float32), band_values)
        return attended.astype(jnp.bfloat16).reshape(WINDOW_REACH, QUERY_HEADS * HEAD_SIZE)
    attended = lax.map(one_block, (grouped_queries, key_matrix[:-1], key_matrix[1:], value_matrix[:-1], value_matrix[1:], key_docs[:-1], key_docs[1:], query_docs))
    attended = attended.reshape(PACK_TOKENS, QUERY_HEADS * HEAD_SIZE)
    projected = jnp.dot(attended.astype(jnp.float32), out_weight.astype(jnp.float32), preferred_element_type=jnp.float32)
    mixed = rounded(residual.astype(jnp.float32) + rounded(projected).astype(jnp.float32))
    widened = mixed.astype(jnp.float32)
    normed = (widened * lax.rsqrt(lax.optimization_barrier(jnp.mean(widened * widened, axis=-1, keepdims=True)) + epsilon) * norm_gain.astype(jnp.float32)).astype(jnp.bfloat16)
    down_groups = down_weight.astype(jnp.float32).reshape(N_TP, FF_DEV, D)

    def mixer_block(rows):
        before = jnp.dot(rows.astype(jnp.float32), up_weight.astype(jnp.float32), preferred_element_type=jnp.float32)
        hidden = jnp.square(jax.nn.relu(before)).astype(jnp.bfloat16)
        parts = jnp.einsum('rnf,nfd->nrd', hidden.reshape(rows.shape[0], N_TP, FF_DEV).astype(jnp.float32), down_groups)
        return lax.optimization_barrier(jnp.sum(rounded(parts).astype(jnp.float32), axis=0))
    branch = lax.map(mixer_block, normed.reshape(N_SP, TOK_DEV, D)).reshape(PACK_TOKENS, D)
    return (widened + rounded(branch).astype(jnp.float32)).astype(jnp.bfloat16)
```

```python
import jax
import jax.numpy as jnp
from jax import lax
from jax.sharding import PartitionSpec as P

HEAD_SIZE = 64
WINDOW_REACH = 128


masked_score = -1e30
epsilon = 1e-06


def passed_along(shard, axis, by):
    peers = lax.axis_size(axis)
    pairs = [(i, i + by) for i in range(peers) if 0 <= i + by < peers]
    return lax.ppermute(shard, axis, pairs)


def turned(shard, axis, by):
    peers = lax.axis_size(axis)
    return lax.ppermute(shard, axis, [(i, (i + by) % peers) for i in range(peers)])


def rounded(value):
    return lax.optimization_barrier(value.astype(jnp.bfloat16))


def squared_relu(before):
    return jnp.square(jax.nn.relu(before)).astype(jnp.bfloat16)


def windowed_attention(queries, keys, values, documents, sinks):
    length = queries.shape[0]
    heads = queries.shape[1] // HEAD_SIZE
    kv_heads = keys.shape[1] // HEAD_SIZE
    query_group = heads // kv_heads
    block_list = length // WINDOW_REACH
    prev_keys, prev_values, prev_docs = passed_along(
        (
            keys[length - WINDOW_REACH :],
            values[length - WINDOW_REACH :],
            documents[length - WINDOW_REACH :],
        ),
        "sp",
        1,
    )
    offset = lax.axis_index("sp") * length
    key_matrix = jnp.concatenate([prev_keys, keys], axis=0).reshape(
        block_list + 1, WINDOW_REACH, kv_heads, HEAD_SIZE
    )
    value_matrix = jnp.concatenate([prev_values, values], axis=0).reshape(
        block_list + 1, WINDOW_REACH, kv_heads, HEAD_SIZE
    )
    key_docs = jnp.concatenate([prev_docs, documents], axis=0).reshape(block_list + 1, WINDOW_REACH)
    key_place = (
        offset - WINDOW_REACH + jnp.arange((block_list + 1) * WINDOW_REACH, dtype=jnp.int32)
    ).reshape(block_list + 1, WINDOW_REACH)
    band_keys = jnp.concatenate([key_matrix[:-1], key_matrix[1:]], axis=1)
    band_values = jnp.concatenate([value_matrix[:-1], value_matrix[1:]], axis=1)
    band_docs = jnp.concatenate([key_docs[:-1], key_docs[1:]], axis=1)
    band_place = jnp.concatenate([key_place[:-1], key_place[1:]], axis=1)
    query_docs = documents.reshape(block_list, WINDOW_REACH)
    grouped_queries = queries.reshape(block_list, WINDOW_REACH, kv_heads, query_group, HEAD_SIZE)
    scores = jnp.einsum(
        "nqhgd,nshd->nhgqs", grouped_queries, band_keys, preferred_element_type=jnp.float32
    ) * HEAD_SIZE ** (-0.5)
    row_index = jnp.arange(WINDOW_REACH, dtype=jnp.int32)[:, None]
    col_index = jnp.arange(2 * WINDOW_REACH, dtype=jnp.int32)[None, :]
    distance = WINDOW_REACH + row_index - col_index
    near = (distance >= 0) & (distance < WINDOW_REACH)
    visible = (
        near[None]
        & (band_docs[:, None, :] == query_docs[:, :, None])
        & (band_place[:, None, :] >= 0)
    )
    visible = visible[:, None, None]
    head_sink_logit = sinks.reshape(kv_heads, query_group)[None, :, :, None]
    scores = jnp.where(visible, scores, masked_score)
    top = jnp.maximum(jnp.max(scores, axis=-1), head_sink_logit)
    exponent = jnp.where(visible, jnp.exp(scores - top[..., None]), 0.0)
    total = jnp.exp(head_sink_logit - top) + jnp.sum(exponent, axis=-1)
    shares = (exponent / total[..., None]).astype(jnp.bfloat16)
    attended = jnp.einsum(
        "nhgqs,nshd->nqhgd", shares, band_values, preferred_element_type=jnp.float32
    )
    return attended.astype(jnp.bfloat16).reshape(length, heads * HEAD_SIZE)


def gathered_rows(rows, axis):
    peers = lax.axis_size(axis)
    place = lax.axis_index(axis)
    count = rows.shape[0]
    whole = jnp.zeros((peers * count, rows.shape[1]), rows.dtype)
    for by in range(peers):
        piece = turned(rows, axis, by) if by else rows
        whole = lax.dynamic_update_slice(whole, piece, (((place - by) % peers) * count, 0))
    return whole


def scattered_sum(partial, axis):
    peers = lax.axis_size(axis)
    place = lax.axis_index(axis)
    count = partial.shape[0] // peers
    total = None
    for by in range(peers):
        piece = lax.dynamic_slice(
            partial, (((place + by) % peers) * count, 0), (count, partial.shape[1])
        )
        piece = (turned(piece, axis, by) if by else piece).astype(jnp.float32)
        total = piece if total is None else total + piece
    return total


def body(
    queries, keys, values, documents, sinks, out_weight, residual, norm_gain, up_weight, down_weight
):
    up_whole = lax.all_gather(up_weight, "sp", axis=0, tiled=True)
    down_whole = lax.all_gather(down_weight, "sp", axis=1, tiled=True)
    attended = windowed_attention(queries, keys, values, documents, sinks)
    token_heads = lax.all_to_all(attended, "tp", split_axis=0, concat_axis=1, tiled=True)
    projected = jnp.dot(token_heads, out_weight, preferred_element_type=jnp.float32)
    mixed = rounded(residual.astype(jnp.float32) + rounded(projected).astype(jnp.float32))
    widened = mixed.astype(jnp.float32)
    normed = (
        widened
        * lax.rsqrt(jnp.mean(widened * widened, axis=-1, keepdims=True) + epsilon)
        * norm_gain
    ).astype(jnp.bfloat16)
    hidden = squared_relu(
        jnp.dot(gathered_rows(normed, "tp"), up_whole, preferred_element_type=jnp.float32)
    )
    partial = jnp.dot(hidden, down_whole, preferred_element_type=jnp.float32).astype(jnp.bfloat16)
    branch = scattered_sum(partial, "tp")
    return (widened + rounded(branch).astype(jnp.float32)).astype(jnp.bfloat16)


def solution(mesh):
    in_specs = (
        P("sp", "tp"),
        P("sp", "tp"),
        P("sp", "tp"),
        P("sp"),
        P("tp"),
        P(),
        P(("sp", "tp"), None),
        P(),
        P("sp", "tp"),
        P("tp", "sp"),
    )
    out_specs = P(("sp", "tp"), None)
    return jax.shard_map(body, mesh=mesh, in_specs=in_specs, out_specs=out_specs, check_vma=False)
```

```python
import math

import jax
import jax.numpy as jnp
from jax import lax
from jax.experimental import pallas as pl
from jax.experimental.pallas import tpu as pltpu
from jax.sharding import PartitionSpec as P


HEAD_SIZE = 64
WINDOW_REACH = 128


masked_score = -1e30
epsilon = 1e-06
MIB = 1 << 20


class Grid:
    def __init__(self):
        peers, self.ny = lax.axis_size("sp"), lax.axis_size("tp")
        self.nc = 2
        chips = peers // self.nc
        self.nx = math.isqrt(chips // 2)
        self.nz = chips // self.nx
        self.ring = [2 * p if 2 * p < self.nz else 2 * (self.nz - 1 - p) + 1 for p in range(self.nz)]
        sp = lax.axis_index("sp")
        self.c = sp % self.nc
        self.x = (sp // self.nc) % self.nx
        self.z = sp // (self.nc * self.nx)
        self.pos = jnp.where(self.z % 2 == 0, self.z // 2, self.nz - 1 - self.z // 2)

    def send(self, value, dz=0, dx=0, dc=0, dy=0):
        pairs = []
        for p in range(self.nz):
            for x in range(self.nx):
                for c in range(self.nc):
                    for y in range(self.ny):
                        pairs.append(
                            (
                                self.line(self.ring[p], x, c, y),
                                self.line(
                                    self.ring[(p + dz) % self.nz],
                                    (x + dx) % self.nx,
                                    (c + dc) % self.nc,
                                    (y + dy) % self.ny,
                                ),
                            )
                        )
        return lax.ppermute(value, ("sp", "tp"), pairs)

    def line(self, z, x, c, y):
        return ((z * self.nx + x) * self.nc + c) * self.ny + y

    def ring_z(self, step):
        p = (self.pos - step) % self.nz
        return jnp.where(2 * p < self.nz, 2 * p, 2 * (self.nz - 1 - p) + 1)


def passed_along(shard, axis, by):
    peers = lax.axis_size(axis)
    pairs = [(i, i + by) for i in range(peers) if 0 <= i + by < peers]
    return lax.ppermute(shard, axis, pairs)


def rounded(value):
    return lax.optimization_barrier(value.astype(jnp.bfloat16))


def spec(kind=None):
    return pl.BlockSpec(memory_space=pltpu.SMEM if kind == "scalar" else pltpu.VMEM)


def attention_kernel(turn_ref, sinks_ref, docs_ref, q_ref, k_ref, v_ref, halo_ref, *rest):
    outs, whole_ref = rest[:-1], rest[-1]
    length, kv_width = k_ref.shape
    kv_heads = kv_width // HEAD_SIZE
    group = q_ref.shape[1] // kv_width
    reach = WINDOW_REACH
    key = lax.broadcasted_iota(jnp.int32, (2 * reach, reach), 0)
    query = lax.broadcasted_iota(jnp.int32, (2 * reach, reach), 1)
    distance = reach + query - key
    near = (distance >= 0) & (distance < reach)
    halo_docs = [
        halo_ref[2 * reach + start // kv_width * 16 :, :][:1, :] for start in range(0, reach, kv_width)
    ]
    halo_docs = jnp.concatenate(halo_docs, axis=1).astype(jnp.float32)
    halo_docs = jnp.where(turn_ref[len(outs)] == 0, -1.0, halo_docs)
    docs = docs_ref[...].astype(jnp.float32)
    rows = [jnp.broadcast_to(halo_docs, (reach, reach))]
    rows += [jnp.broadcast_to(docs[n : n + 1, :], (reach, reach)) for n in range(length // reach)]
    columns = [row.T for row in rows]
    for n in range(length // reach):
        here = slice(n * reach, (n + 1) * reach)
        back = slice((n - 1) * reach, n * reach)
        same = jnp.concatenate([columns[n], columns[n + 1]], axis=0) == jnp.concatenate(
            [rows[n + 1]] * 2, axis=0
        )
        hide = jnp.where(near & same, 0.0, masked_score)
        hide = jnp.concatenate([hide] * group, axis=1)
        early_k = k_ref[back, :] if n else halo_ref[:reach, :]
        early_v = v_ref[back, :] if n else halo_ref[reach : 2 * reach, :]
        band_k = jnp.concatenate([early_k, k_ref[here, :]], axis=0)
        band_v = jnp.concatenate([early_v, v_ref[here, :]], axis=0)
        for h in range(kv_heads):
            kv = slice(h * HEAD_SIZE, (h + 1) * HEAD_SIZE)
            heads = [h * group + g for g in range(group)]
            q = jnp.concatenate(
                [q_ref[here, i * HEAD_SIZE : (i + 1) * HEAD_SIZE] for i in heads], axis=0
            )
            scores = lax.dot_general(
                band_k[:, kv], q, (((1,), (1,)), ((), ())), preferred_element_type=jnp.float32
            ) * HEAD_SIZE ** (-0.5)
            scores = jnp.where(hide < 0.0, masked_score, scores)
            sink = jnp.concatenate(
                [jnp.full((1, reach), sinks_ref[i], jnp.float32) for i in heads], axis=1
            )
            top = jnp.maximum(jnp.max(scores, axis=0, keepdims=True), sink)
            exponent = jnp.exp(scores - top)
            total = jnp.exp(sink - top) + jnp.sum(exponent, axis=0, keepdims=True)
            shares = (exponent * (1.0 / total)).astype(jnp.bfloat16)
            attended = lax.dot_general(
                band_v[:, kv], shares, (((0,), (0,)), ((), ())), preferred_element_type=jnp.float32
            )
            for g, i in enumerate(heads):
                whole_ref[here, i * HEAD_SIZE : (i + 1) * HEAD_SIZE] = attended[
                    :, g * reach : (g + 1) * reach
                ].T.astype(jnp.bfloat16)
    count = outs[0].shape[0]
    for dy, out in enumerate(outs):
        out[...] = whole_ref[pl.ds(pl.multiple_of(turn_ref[dy] * count, count), count), :]


def prepare_kernel(turn_ref, docs_ref, k_ref, v_ref, up_ref, halo_ref, *refs):
    parts, sems = refs[:-1], refs[-1]
    reach, kv_width = WINDOW_REACH, k_ref.shape[1]
    last = k_ref.shape[0] - reach
    width = parts[0].shape[1]
    copies = []
    for i, part in enumerate(parts):
        start = pl.multiple_of(turn_ref[i] * width, width)
        copies.append(
            pltpu.make_async_copy(up_ref.at[:, pl.ds(start, width)], part, sems.at[i])
        )
    for i, ref in enumerate((k_ref, v_ref)):
        to = halo_ref.at[pl.ds(i * reach, reach), :]
        copies.append(
            pltpu.make_async_copy(ref.at[pl.ds(last, reach), :], to, sems.at[len(parts) + i])
        )
    for copy in copies:
        copy.start()
    docs = docs_ref[docs_ref.shape[0] - 1 :, :].astype(jnp.float32).astype(jnp.bfloat16)
    for start in range(0, reach, kv_width):
        row = docs[:, start : start + kv_width]
        at = 2 * reach + start // kv_width * 16
        halo_ref[at : at + 16, :] = jnp.broadcast_to(row, (16, kv_width))
    for copy in copies:
        copy.wait()


def prepare(grid, keys, values, documents, up_weight, width):
    kv_width = keys.shape[1]
    part = jax.ShapeDtypeStruct((up_weight.shape[0], width), up_weight.dtype)
    docs_rows = 16 * (WINDOW_REACH // kv_width)
    halo = jax.ShapeDtypeStruct((2 * WINDOW_REACH + docs_rows, kv_width), keys.dtype)
    turn = jnp.stack([(grid.x + dx) % grid.nx for dx in range(grid.nx)])
    far = pl.BlockSpec(memory_space=pltpu.HBM)
    return pl.pallas_call(
        prepare_kernel,
        out_shape=[halo] + [part] * grid.nx,
        in_specs=[spec("scalar"), spec()] + [far] * 3,
        out_specs=[spec()] * (1 + grid.nx),
        scratch_shapes=[pltpu.SemaphoreType.DMA((grid.nx + 2,))],
        compiler_params=pltpu.CompilerParams(vmem_limit_bytes=60 * MIB),
    )(turn, documents.reshape(-1, WINDOW_REACH), keys, values, up_weight)


def windowed_attention(grid, halo, queries, keys, values, documents, sinks):
    length = queries.shape[0]
    halo = passed_along(halo, "sp", 1)
    turn = [(lax.axis_index("tp") + dy) % grid.ny for dy in range(grid.ny)]
    turn = jnp.stack(turn + [lax.axis_index("sp")])
    piece = jax.ShapeDtypeStruct((length // grid.ny, queries.shape[1]), jnp.bfloat16)
    return pl.pallas_call(
        attention_kernel,
        out_shape=[piece] * grid.ny,
        in_specs=[spec("scalar")] * 2 + [spec()] * 5,
        out_specs=[spec()] * grid.ny,
        scratch_shapes=[pltpu.VMEM(queries.shape, jnp.bfloat16)],
        compiler_params=pltpu.CompilerParams(vmem_limit_bytes=8 * MIB),
    )(turn, sinks, documents.reshape(-1, WINDOW_REACH), queries, keys, values, halo)


def project_kernel(place_ref, *refs):
    pieces = refs[:-5]
    weight_ref, residual_ref, gain_ref, mixed_ref, normed_ref = refs[-5:]
    width = pieces[0].shape[1]
    total = None
    for i, piece in enumerate(pieces):
        start = pl.multiple_of(place_ref[i] * width, width)
        part = jnp.dot(
            piece[...], weight_ref[pl.ds(start, width), :], preferred_element_type=jnp.float32
        )
        total = part if total is None else total + part
    projected = total.astype(jnp.bfloat16).astype(jnp.float32)
    mixed = (residual_ref[...].astype(jnp.float32) + projected).astype(jnp.bfloat16)
    mixed_ref[...] = mixed
    widened = mixed.astype(jnp.float32)
    scale = lax.rsqrt(jnp.mean(widened * widened, axis=-1, keepdims=True) + epsilon)
    normed_ref[...] = (widened * scale * gain_ref[...]).astype(jnp.bfloat16)


def project(places, pieces, out_weight, residual, norm_gain):
    rows = jax.ShapeDtypeStruct(residual.shape, jnp.bfloat16)
    return pl.pallas_call(
        project_kernel,
        out_shape=[rows, rows],
        in_specs=[spec("scalar")] + [spec()] * (len(pieces) + 3),
        out_specs=[spec()] * 2,
        compiler_params=pltpu.CompilerParams(vmem_limit_bytes=16 * MIB),
    )(places, *pieces, out_weight, residual, norm_gain.reshape(1, -1))


def chosen_columns(place_ref, places, rows, tokens, out_ref):
    count = tokens[0].shape[0]
    for g, x_ref in enumerate(tokens):
        for i, place in enumerate(places):
            start = pl.multiple_of(place_ref[place] * rows, rows)
            out_ref[g * count : (g + 1) * count, i * rows : (i + 1) * rows] = x_ref[
                :, pl.ds(start, rows)
            ]


def joined_rows(held, out_ref):
    rows = held[0].shape[0]
    for i, piece in enumerate(held):
        out_ref[i * rows : (i + 1) * rows, :] = piece[...]


def up_early_kernel(place_ref, *refs, groups, pieces):
    tokens, held = refs[:groups], refs[groups : groups + pieces]
    *before_refs, whole_ref, columns_ref = refs[groups + pieces :]
    joined_rows(held, whole_ref)
    chosen_columns(place_ref, range(pieces), held[0].shape[0], tokens, columns_ref)
    step = before_refs[0].shape[1]
    for i, before_ref in enumerate(before_refs):
        before_ref[...] = jnp.dot(
            columns_ref[...],
            whole_ref[:, i * step : (i + 1) * step],
            preferred_element_type=jnp.float32,
        )


def up_late_kernel(place_ref, *refs, groups, pieces, early, first):
    tokens, held = refs[:groups], refs[groups : groups + pieces]
    *early_refs, whole_ref, columns_ref = refs[groups + pieces :]
    early_refs, units_refs = early_refs[:early], early_refs[early:]
    joined_rows(held, whole_ref)
    places = range(first, first + pieces)
    chosen_columns(place_ref, places, held[0].shape[0], tokens, columns_ref)
    step = early_refs[0].shape[1]
    for i, early_ref in enumerate(early_refs):
        cols = slice(i * step, (i + 1) * step)
        before = early_ref[...] + jnp.dot(
            columns_ref[...], whole_ref[:, cols], preferred_element_type=jnp.float32
        )
        units = jnp.square(jnp.maximum(before, 0.0)).astype(jnp.bfloat16)
        held_width = units_refs[0].shape[1]
        at = i * step % held_width
        units_refs[i * step // held_width][:, at : at + step] = units


def up_far_kernel(place_ref, *refs, rows, pieces):
    tokens = refs[:-5]
    early_ref, late_ref, units_ref, full_ref, columns_ref = refs[-5:]
    begin = 0
    for x_ref in tokens:
        full_ref[:, begin : begin + x_ref.shape[1]] = x_ref[...]
        begin += x_ref.shape[1]
    chosen_columns(place_ref, range(pieces), rows, [full_ref], columns_ref)
    cut, width = early_ref.shape
    step = min(width, 512)
    for start in range(0, width, step):
        cols = slice(start, start + step)
        before = jnp.dot(
            columns_ref[:, :cut], early_ref[:, cols], preferred_element_type=jnp.float32
        )
        before += jnp.dot(
            columns_ref[:, cut:], late_ref[:, cols], preferred_element_type=jnp.float32
        )
        units_ref[:, cols] = jnp.square(jnp.maximum(before, 0.0)).astype(jnp.bfloat16)


def limit(mebibytes):
    return pltpu.CompilerParams(vmem_limit_bytes=mebibytes * MIB)


def up_early(places, tokens, held):
    rows, width = held[0].shape
    step = min(width, 512)
    count = sum(x.shape[0] for x in tokens)
    depth = rows * len(held)

    def kernel(*refs):
        up_early_kernel(*refs, groups=len(tokens), pieces=len(held))

    return pl.pallas_call(
        kernel,
        out_shape=[jax.ShapeDtypeStruct((count, step), jnp.float32)] * (width // step)
        + [jax.ShapeDtypeStruct((depth, width), jnp.bfloat16)],
        in_specs=[spec("scalar")] + [spec()] * (len(tokens) + len(held)),
        out_specs=[spec()] * (width // step + 1),
        scratch_shapes=[pltpu.VMEM((count, depth), jnp.bfloat16)],
        compiler_params=limit(30),
    )(places, *tokens, *held)


def up_late(places, tokens, held, early, first):
    rows, width = held[0].shape
    count = sum(x.shape[0] for x in tokens)
    depth = rows * len(held)
    halves = 4

    def kernel(*refs):
        up_late_kernel(
            *refs, groups=len(tokens), pieces=len(held), early=len(early), first=first
        )

    return pl.pallas_call(
        kernel,
        out_shape=[jax.ShapeDtypeStruct((count, width // halves), jnp.bfloat16)] * halves
        + [jax.ShapeDtypeStruct((depth, width), jnp.bfloat16)],
        in_specs=[spec("scalar")] + [spec()] * (len(tokens) + len(held) + len(early)),
        out_specs=[spec()] * (halves + 1),
        scratch_shapes=[pltpu.VMEM((count, depth), jnp.bfloat16)],
        compiler_params=limit(22),
    )(places, *tokens, *held, *early)


def up_far(places, tokens, early, late, rows):
    count, model = tokens[0].shape[0], early.shape[0] + late.shape[0]

    def kernel(*refs):
        up_far_kernel(*refs, rows=rows, pieces=model // rows)

    return pl.pallas_call(
        kernel,
        out_shape=jax.ShapeDtypeStruct((count, early.shape[1]), jnp.bfloat16),
        in_specs=[spec("scalar")] + [spec()] * (len(tokens) + 2),
        out_specs=spec(),
        scratch_shapes=[pltpu.VMEM((count, model), jnp.bfloat16)] * 2,
        compiler_params=limit(16),
    )(places, *tokens, early, late)


def up_kernel(place_ref, *refs, groups, pieces):
    tokens, held = refs[:groups], refs[groups : groups + pieces]
    units_ref, whole_ref = refs[groups + pieces :]
    rows, count = held[0].shape[0], tokens[0].shape[0]
    for i, piece in enumerate(held):
        whole_ref[pl.ds(pl.multiple_of(place_ref[i] * rows, rows), rows), :] = piece[...]
    for g, x_ref in enumerate(tokens):
        before = jnp.dot(x_ref[...], whole_ref[...], preferred_element_type=jnp.float32)
        units = jnp.square(jnp.maximum(before, 0.0)).astype(jnp.bfloat16)
        units_ref[g * count : (g + 1) * count, :] = units


def up_whole(places, tokens, held):
    rows, width = held[0].shape

    def kernel(*refs):
        up_kernel(*refs, groups=len(tokens), pieces=len(held))

    return pl.pallas_call(
        kernel,
        out_shape=jax.ShapeDtypeStruct((sum(x.shape[0] for x in tokens), width), jnp.bfloat16),
        in_specs=[spec("scalar")] + [spec()] * (len(tokens) + len(held)),
        out_specs=spec(),
        scratch_shapes=[pltpu.VMEM((rows * len(held), width), jnp.bfloat16)],
        compiler_params=limit(32),
    )(places, *tokens, *held)


def down_kernel(*refs, parts, pieces):
    units = sum(parts)
    hidden, held = refs[:units], refs[units : units + pieces]
    outs, whole_ref = refs[units + pieces : -1], refs[-1]
    cols, count = held[0].shape[1], outs[0].shape[0]
    for i, piece in enumerate(held):
        whole_ref[:, i * cols : (i + 1) * cols] = piece[...]
    at = out = 0
    for part in parts:
        total, begin = None, 0
        for unit in hidden[at : at + part]:
            end = begin + unit.shape[1]
            term = jnp.dot(
                unit[...], whole_ref[begin:end, :], preferred_element_type=jnp.float32
            )
            total, begin = term if total is None else total + term, end
        at += part
        for start in range(0, total.shape[0], count):
            outs[out][...] = total[start : start + count, :].astype(jnp.bfloat16)
            out += 1


def down_project(hidden, held, groups):
    width, cols = held[0].shape
    count = sum(parts[0].shape[0] for parts in hidden) // groups
    out = jax.ShapeDtypeStruct((count, cols * len(held)), jnp.bfloat16)
    flat = [unit for parts in hidden for unit in parts]

    def kernel(*refs):
        down_kernel(*refs, parts=[len(parts) for parts in hidden], pieces=len(held))

    return pl.pallas_call(
        kernel,
        out_shape=[out] * groups,
        in_specs=[spec()] * (len(flat) + len(held)),
        out_specs=[spec()] * groups,
        scratch_shapes=[pltpu.VMEM((width, cols * len(held)), jnp.bfloat16)],
        compiler_params=limit(14),
    )(*flat, *held)


def layer(
    queries, keys, values, documents, sinks, out_weight, residual, norm_gain, up_weight, down_weight
):
    grid = Grid()
    nx, ny, nz, nc = grid.nx, grid.ny, grid.nz, grid.nc
    rows, width = up_weight.shape[0], up_weight.shape[1] // nx

    halo, *up_parts = prepare(grid, keys, values, documents, up_weight, width)
    up_blocks, down_blocks = [], []
    for dx in range(nx):
        up_part = up_parts[dx]
        part = ((grid.x + dx) % nx) * width
        down_part = lax.dynamic_slice(down_weight, (part, 0), (width, rows))
        up_blocks.append(grid.send(up_part, dx=dx) if dx else up_part)
        down_blocks.append(grid.send(down_part, dx=dx) if dx else down_part)

    up_held, up_places = [], []
    for step in range(nz):
        for dx in range(nx):
            if step:
                up_blocks[dx] = grid.send(up_blocks[dx], dz=1)
            chip = grid.ring_z(step) * nx + (grid.x - dx) % nx
            for dc in range(nc):
                up_held.append(grid.send(up_blocks[dx], dc=dc) if dc else up_blocks[dx])
                up_places.append(chip * nc + (grid.c - dc) % nc)
    up_places = jnp.stack(up_places)

    down_held = []
    for x in range(nx):
        held = down_blocks[0]
        for dx in range(1, nx):
            held = jnp.where((grid.x - dx) % nx == x, down_blocks[dx], held)
        down_held.append(held)

    pieces = windowed_attention(grid, halo, queries, keys, values, documents, sinks)
    heads = []
    for dy in range(ny):
        heads.append(grid.send(pieces[dy], dy=dy) if dy else pieces[dy])
    places = jnp.stack([(lax.axis_index("tp") - dy) % ny for dy in range(ny)])
    mixed, normed = project(places, heads, out_weight, residual, norm_gain)

    groups = [(dx, dy) for dx in range(nx) for dy in range(ny)]
    groups.sort(key=lambda group: (group[0] > 0) + (group[1] > 0))
    tokens = {}
    for dx, dy in groups:
        if dx and dy and nx == ny == 2 and rows % 128 == 0:
            half = normed.shape[1] // 2
            left = grid.send(tokens[0, 1][0][:, :half], dx=1)
            right = grid.send(tokens[1, 0][0][:, half:], dy=1)
            tokens[dx, dy] = (left, right)
            continue
        tokens[dx, dy] = (grid.send(normed, dx=dx, dy=dy) if dx or dy else normed,)
    tokens = [tokens[group] for group in groups]
    near = sum(1 for dx, dy in groups if not (dx and dy))
    near_tokens = [part[0] for part in tokens[:near]]
    if rows % 128 == 0 and near == len(groups) - 1:
        first = (nz - 1) * nx * nc
        *before, early = up_early(up_places, near_tokens, up_held[:first])
        *units, late = up_late(up_places, near_tokens, up_held[first:], before, first)
        hidden = [units, [up_far(up_places, tokens[-1], early, late, rows)]]
    else:
        hidden = [[up_whole(up_places, near_tokens, up_held)]]
        if near < len(groups):
            far_tokens = [part[0] for part in tokens[near:]]
            hidden.append([up_whole(up_places, far_tokens, up_held)])

    every, per = list(range(nx)), max(1, nz // 4)
    chunks = [(list(range(s, s + per)), every) for s in range(0, nz, per)]
    if nx == 2:
        chunks[-2:] = [(steps, [x]) for steps, _ in chunks[-2:] for x in every]
    columns = {}
    for step in range(nz):
        for x in range(nx):
            if step:
                down_held[x] = grid.send(down_held[x], dz=1)
            for dc in range(nc):
                columns[step, x, dc] = grid.send(down_held[x], dc=dc) if dc else down_held[x]
    out = mixed
    for steps, span in chunks:
        held = [columns[step, x, dc] for step in steps for x in span for dc in range(nc)]
        partial = down_project(hidden, held, len(groups))
        terms = []
        for (dx, dy), piece in zip(groups, partial):
            terms.append(grid.send(piece, dx=-dx, dy=-dy) if dx or dy else piece)
        branch = rounded(sum(term.astype(jnp.float32) for term in terms)).astype(jnp.float32)
        blocks = jnp.split(branch, len(held), axis=1)
        ordered = []
        for i in range(0, len(blocks), nc):
            for c in range(nc):
                block = blocks[i]
                for dc in range(1, nc):
                    block = jnp.where((grid.c - dc) % nc == c, blocks[i + dc], block)
                ordered.append(block)
        each = len(span) * nc
        for i, step in enumerate(steps):
            part = jnp.concatenate(ordered[i * each : (i + 1) * each], axis=1)
            place = ((grid.ring_z(step) * nx + span[0]) * nc) * rows
            before = lax.dynamic_slice(mixed, (0, place), (mixed.shape[0], part.shape[1]))
            after = (before.astype(jnp.float32) + part).astype(jnp.bfloat16)
            out = lax.dynamic_update_slice(out, after, (0, place))
    return out


def solution(mesh):
    in_specs = (
        P("sp", "tp"),
        P("sp", "tp"),
        P("sp", "tp"),
        P("sp"),
        P("tp"),
        P(),
        P(("sp", "tp"), None),
        P(),
        P("sp", "tp"),
        P("tp", "sp"),
    )
    out_specs = P(("sp", "tp"), None)
    return jax.shard_map(layer, mesh=mesh, in_specs=in_specs, out_specs=out_specs, check_vma=False)
```

```python
import functools
import math

import jax
import jax.numpy as jnp
from jax import lax
from jax.experimental import pallas as pl
from jax.experimental.pallas import tpu as pltpu
from jax.sharding import PartitionSpec as P


HEAD_SIZE = 64
WINDOW_REACH = 128


masked_score = -1e30
epsilon = 1e-06
MIB = 1 << 20


class Grid:
    def __init__(self):
        peers, self.ny = lax.axis_size("sp"), lax.axis_size("tp")
        self.nc = 2
        chips = peers // self.nc
        self.nx = math.isqrt(chips // 2)
        self.nz = chips // self.nx
        self.ring = [2 * p if 2 * p < self.nz else 2 * (self.nz - 1 - p) + 1 for p in range(self.nz)]
        sp = lax.axis_index("sp")
        self.c = sp % self.nc
        self.x = (sp // self.nc) % self.nx
        self.z = sp // (self.nc * self.nx)
        self.pos = jnp.where(self.z % 2 == 0, self.z // 2, self.nz - 1 - self.z // 2)

    def send(self, value, dz=0, dx=0, dc=0, dy=0):
        pairs = []
        for p in range(self.nz):
            for x in range(self.nx):
                for c in range(self.nc):
                    for y in range(self.ny):
                        pairs.append(
                            (
                                self.line(self.ring[p], x, c, y),
                                self.line(
                                    self.ring[(p + dz) % self.nz],
                                    (x + dx) % self.nx,
                                    (c + dc) % self.nc,
                                    (y + dy) % self.ny,
                                ),
                            )
                        )
        return lax.ppermute(value, ("sp", "tp"), pairs)

    def line(self, z, x, c, y):
        return ((z * self.nx + x) * self.nc + c) * self.ny + y

    def ring_z(self, step):
        p = (self.pos - step) % self.nz
        return jnp.where(2 * p < self.nz, 2 * p, 2 * (self.nz - 1 - p) + 1)


def passed_along(shard, axis, by):
    peers = lax.axis_size(axis)
    pairs = [(i, i + by) for i in range(peers) if 0 <= i + by < peers]
    return lax.ppermute(shard, axis, pairs)


def rounded(value):
    return lax.optimization_barrier(value.astype(jnp.bfloat16))


def spec(kind=None):
    return pl.BlockSpec(memory_space=pltpu.SMEM if kind == "scalar" else pltpu.VMEM)


def attention_kernel(turn_ref, sinks_ref, docs_ref, q_ref, k_ref, v_ref, halo_ref, *rest):
    outs, whole_ref = rest[:-1], rest[-1]
    length, kv_width = k_ref.shape
    kv_heads = kv_width // HEAD_SIZE
    group = q_ref.shape[1] // kv_width
    reach = WINDOW_REACH
    key = lax.broadcasted_iota(jnp.int32, (2 * reach, reach), 0)
    query = lax.broadcasted_iota(jnp.int32, (2 * reach, reach), 1)
    distance = reach + query - key
    near = (distance >= 0) & (distance < reach)
    halo_docs = [
        halo_ref[2 * reach + start // kv_width * 16 :, :][:1, :] for start in range(0, reach, kv_width)
    ]
    halo_docs = jnp.concatenate(halo_docs, axis=1).astype(jnp.float32)
    halo_docs = jnp.where(turn_ref[len(outs)] == 0, -1.0, halo_docs)
    docs = docs_ref[...].astype(jnp.float32)
    rows = [jnp.broadcast_to(halo_docs, (reach, reach))]
    rows += [jnp.broadcast_to(docs[n : n + 1, :], (reach, reach)) for n in range(length // reach)]
    columns = [row.T for row in rows]
    for n in range(length // reach):
        here = slice(n * reach, (n + 1) * reach)
        back = slice((n - 1) * reach, n * reach)
        same = jnp.concatenate([columns[n], columns[n + 1]], axis=0) == jnp.concatenate(
            [rows[n + 1]] * 2, axis=0
        )
        hide = jnp.where(near & same, 0.0, masked_score)
        hide = jnp.concatenate([hide] * group, axis=1)
        early_k = k_ref[back, :] if n else halo_ref[:reach, :]
        early_v = v_ref[back, :] if n else halo_ref[reach : 2 * reach, :]
        band_k = jnp.concatenate([early_k, k_ref[here, :]], axis=0)
        band_v = jnp.concatenate([early_v, v_ref[here, :]], axis=0)
        for h in range(kv_heads):
            kv = slice(h * HEAD_SIZE, (h + 1) * HEAD_SIZE)
            heads = [h * group + g for g in range(group)]
            q = jnp.concatenate(
                [q_ref[here, i * HEAD_SIZE : (i + 1) * HEAD_SIZE] for i in heads], axis=0
            )
            scores = lax.dot_general(
                band_k[:, kv], q, (((1,), (1,)), ((), ())), preferred_element_type=jnp.float32
            ) * HEAD_SIZE ** (-0.5)
            scores = jnp.where(hide < 0.0, masked_score, scores)
            sink = jnp.concatenate(
                [jnp.full((1, reach), sinks_ref[i], jnp.float32) for i in heads], axis=1
            )
            top = jnp.maximum(jnp.max(scores, axis=0, keepdims=True), sink)
            exponent = jnp.exp(scores - top)
            total = jnp.exp(sink - top) + jnp.sum(exponent, axis=0, keepdims=True)
            shares = (exponent * (1.0 / total)).astype(jnp.bfloat16)
            attended = lax.dot_general(
                band_v[:, kv], shares, (((0,), (0,)), ((), ())), preferred_element_type=jnp.float32
            )
            for g, i in enumerate(heads):
                whole_ref[here, i * HEAD_SIZE : (i + 1) * HEAD_SIZE] = attended[
                    :, g * reach : (g + 1) * reach
                ].T.astype(jnp.bfloat16)
    count = outs[0].shape[0]
    for dy, out in enumerate(outs):
        out[...] = whole_ref[pl.ds(pl.multiple_of(turn_ref[dy] * count, count), count), :]


def prepare_kernel(turn_ref, docs_ref, k_ref, v_ref, up_ref, halo_ref, *refs, width, units):
    parts, sems = refs[:-1], refs[-1]
    reach, kv_width = WINDOW_REACH, k_ref.shape[1]
    last = k_ref.shape[0] - reach
    copies = []
    for i, (part, (dx, at)) in enumerate(zip(parts, units)):
        start = pl.multiple_of(turn_ref[dx] * width + at * part.shape[1], part.shape[1])
        columns = up_ref.at[:, pl.ds(start, part.shape[1])]
        copies.append(pltpu.make_async_copy(columns, part, sems.at[i]))
    for i, ref in enumerate((k_ref, v_ref)):
        to = halo_ref.at[pl.ds(i * reach, reach), :]
        copies.append(
            pltpu.make_async_copy(ref.at[pl.ds(last, reach), :], to, sems.at[len(parts) + i])
        )
    for copy in copies:
        copy.start()
    docs = docs_ref[docs_ref.shape[0] - 1 :, :].astype(jnp.float32).astype(jnp.bfloat16)
    for start in range(0, reach, kv_width):
        row = docs[:, start : start + kv_width]
        at = 2 * reach + start // kv_width * 16
        halo_ref[at : at + 16, :] = jnp.broadcast_to(row, (16, kv_width))
    for copy in copies:
        copy.wait()


def prepare(grid, keys, values, documents, up_weight, width, units):
    kv_width = keys.shape[1]
    shares = [sum(dx == other for other, _ in units) for dx, _ in units]
    parts = [
        jax.ShapeDtypeStruct((up_weight.shape[0], width // share), up_weight.dtype)
        for share in shares
    ]

    def kernel(*refs):
        prepare_kernel(*refs, width=width, units=units)

    docs_rows = 16 * (WINDOW_REACH // kv_width)
    halo = jax.ShapeDtypeStruct((2 * WINDOW_REACH + docs_rows, kv_width), keys.dtype)
    turn = jnp.stack([(grid.x + dx) % grid.nx for dx in range(grid.nx)])
    far = pl.BlockSpec(memory_space=pltpu.HBM)
    return pl.pallas_call(
        kernel,
        out_shape=[halo] + parts,
        in_specs=[spec("scalar"), spec()] + [far] * 3,
        out_specs=[spec()] * (1 + len(parts)),
        scratch_shapes=[pltpu.SemaphoreType.DMA((len(parts) + 2,))],
        compiler_params=pltpu.CompilerParams(vmem_limit_bytes=60 * MIB),
    )(turn, documents.reshape(-1, WINDOW_REACH), keys, values, up_weight)


def windowed_attention(grid, halo, queries, keys, values, documents, sinks):
    length = queries.shape[0]
    halo = passed_along(halo, "sp", 1)
    turn = [(lax.axis_index("tp") + dy) % grid.ny for dy in range(grid.ny)]
    turn = jnp.stack(turn + [lax.axis_index("sp")])
    piece = jax.ShapeDtypeStruct((length // grid.ny, queries.shape[1]), jnp.bfloat16)
    return pl.pallas_call(
        attention_kernel,
        out_shape=[piece] * grid.ny,
        in_specs=[spec("scalar")] * 2 + [spec()] * 5,
        out_specs=[spec()] * grid.ny,
        scratch_shapes=[pltpu.VMEM(queries.shape, jnp.bfloat16)],
        compiler_params=pltpu.CompilerParams(vmem_limit_bytes=8 * MIB),
    )(turn, sinks, documents.reshape(-1, WINDOW_REACH), queries, keys, values, halo)


def project_kernel(place_ref, *refs):
    pieces = refs[:-6]
    weight_ref, residual_ref, gain_ref, mixed_ref, left_ref, right_ref = refs[-6:]
    width = pieces[0].shape[1]
    total = None
    for i, piece in enumerate(pieces):
        start = pl.multiple_of(place_ref[i] * width, width)
        part = jnp.dot(
            piece[...], weight_ref[pl.ds(start, width), :], preferred_element_type=jnp.float32
        )
        total = part if total is None else total + part
    projected = total.astype(jnp.bfloat16).astype(jnp.float32)
    mixed = (residual_ref[...].astype(jnp.float32) + projected).astype(jnp.bfloat16)
    mixed_ref[...] = mixed
    widened = mixed.astype(jnp.float32)
    scale = lax.rsqrt(jnp.mean(widened * widened, axis=-1, keepdims=True) + epsilon)
    normed = (widened * scale * gain_ref[...]).astype(jnp.bfloat16)
    half = left_ref.shape[1]
    left_ref[...] = normed[:, :half]
    right_ref[...] = normed[:, half:]


def project(places, pieces, out_weight, residual, norm_gain):
    count, model = residual.shape
    rows = jax.ShapeDtypeStruct(residual.shape, jnp.bfloat16)
    half = jax.ShapeDtypeStruct((count, model // 2), jnp.bfloat16)
    return pl.pallas_call(
        project_kernel,
        out_shape=[rows, half, half],
        in_specs=[spec("scalar")] + [spec()] * (len(pieces) + 3),
        out_specs=[spec()] * 3,
        compiler_params=pltpu.CompilerParams(vmem_limit_bytes=16 * MIB),
    )(places, *pieces, out_weight, residual, norm_gain.reshape(1, -1))


def joined_columns(halves, out_ref):
    count, half = halves[0].shape
    for i, x_ref in enumerate(halves):
        at, begin = i // 2 * count, i % 2 * half
        out_ref[at : at + count, begin : begin + half] = x_ref[...]


def chosen_columns(place_ref, places, rows, halves, out_ref):
    count, half = halves[0].shape
    each = half // rows
    for i, place in enumerate(places):

        def copy(side, i=i, place=place):
            start = pl.multiple_of((place_ref[place] - side * each) * rows, rows)
            for g, x_ref in enumerate(halves[side::2]):
                out_ref[g * count : (g + 1) * count, i * rows : (i + 1) * rows] = x_ref[
                    :, pl.ds(start, rows)
                ]

        pl.when(place_ref[place] < each)(functools.partial(copy, 0))
        pl.when(place_ref[place] >= each)(functools.partial(copy, 1))


def joined_rows(held, shares, out_ref, place_ref=None):
    rows, at = held[0].shape[0], 0
    for i, share in enumerate(shares):
        place = i if place_ref is None else place_ref[i]
        start, begin = pl.multiple_of(place * rows, rows), 0
        for piece in held[at : at + share]:
            end = begin + piece.shape[1]
            out_ref[pl.ds(start, rows), begin:end] = piece[...]
            begin = end
        at += share


def flattened(held):
    return [part for piece in held for part in piece], [len(piece) for piece in held]


def up_early_kernel(place_ref, *refs, groups, shares):
    last, pieces = groups + sum(shares), len(shares)
    tokens, held = refs[:groups], refs[groups:last]
    *before_refs, whole_ref, late_ref, columns_ref = refs[last:]
    rows = held[0].shape[0]
    joined_rows(held, shares, whole_ref)
    chosen_columns(place_ref, range(pieces), rows, tokens, columns_ref)
    rest = range(pieces, pieces + late_ref.shape[1] // rows)
    chosen_columns(place_ref, rest, rows, tokens, late_ref)
    step = before_refs[0].shape[1]
    for i, before_ref in enumerate(before_refs):
        before_ref[...] = jnp.dot(
            columns_ref[...],
            whole_ref[:, i * step : (i + 1) * step],
            preferred_element_type=jnp.float32,
        )


def up_late_kernel(columns_ref, *refs, shares, early):
    pieces = sum(shares)
    held, early_refs = refs[:pieces], refs[pieces : pieces + early]
    *units_refs, whole_ref = refs[pieces + early :]
    joined_rows(held, shares, whole_ref)
    step, held_width = early_refs[0].shape[1], units_refs[0].shape[1]
    for i, early_ref in enumerate(early_refs):
        cols = slice(i * step, (i + 1) * step)
        before = early_ref[...] + jnp.dot(
            columns_ref[...], whole_ref[:, cols], preferred_element_type=jnp.float32
        )
        units = jnp.square(jnp.maximum(before, 0.0)).astype(jnp.bfloat16)
        at = i * step % held_width
        units_refs[i * step // held_width][:, at : at + step] = units


def up_far_kernel(place_ref, *refs, rows, pieces):
    tokens = refs[:-4]
    early_ref, late_ref, units_ref, columns_ref = refs[-4:]
    chosen_columns(place_ref, range(pieces), rows, tokens, columns_ref)
    cut, width = early_ref.shape
    step = min(width, 512)
    for start in range(0, width, step):
        cols = slice(start, start + step)
        before = jnp.dot(
            columns_ref[:, :cut], early_ref[:, cols], preferred_element_type=jnp.float32
        )
        before += jnp.dot(
            columns_ref[:, cut:], late_ref[:, cols], preferred_element_type=jnp.float32
        )
        units_ref[:, cols] = jnp.square(jnp.maximum(before, 0.0)).astype(jnp.bfloat16)


def limit(mebibytes):
    return pltpu.CompilerParams(vmem_limit_bytes=mebibytes * MIB)


def up_early(places, tokens, held):
    flat, shares = flattened(held)
    rows, width = flat[0].shape[0], sum(part.shape[1] for part in held[0])
    step = min(width, 512)
    count, model = sum(x.shape[0] for x in tokens) // 2, 2 * tokens[0].shape[1]
    depth = rows * len(held)

    def kernel(*refs):
        up_early_kernel(*refs, groups=len(tokens), shares=shares)

    return pl.pallas_call(
        kernel,
        out_shape=[jax.ShapeDtypeStruct((count, step), jnp.float32)] * (width // step)
        + [jax.ShapeDtypeStruct((depth, width), jnp.bfloat16)]
        + [jax.ShapeDtypeStruct((count, model - depth), jnp.bfloat16)],
        in_specs=[spec("scalar")] + [spec()] * (len(tokens) + len(flat)),
        out_specs=[spec()] * (width // step + 2),
        scratch_shapes=[pltpu.VMEM((count, depth), jnp.bfloat16)],
        compiler_params=limit(30),
    )(places, *tokens, *flat)


def up_late(columns, held, early):
    flat, shares = flattened(held)
    rows, width = flat[0].shape[0], sum(part.shape[1] for part in held[0])
    count = columns.shape[0]
    depth = rows * len(held)
    halves = 4

    def kernel(*refs):
        up_late_kernel(*refs, shares=shares, early=len(early))

    return pl.pallas_call(
        kernel,
        out_shape=[jax.ShapeDtypeStruct((count, width // halves), jnp.bfloat16)] * halves
        + [jax.ShapeDtypeStruct((depth, width), jnp.bfloat16)],
        in_specs=[spec()] * (1 + len(flat) + len(early)),
        out_specs=[spec()] * (halves + 1),
        compiler_params=limit(22),
    )(columns, *flat, *early)


def up_far(places, tokens, early, late, rows):
    count, model = tokens[0].shape[0], early.shape[0] + late.shape[0]

    def kernel(*refs):
        up_far_kernel(*refs, rows=rows, pieces=model // rows)

    return pl.pallas_call(
        kernel,
        out_shape=jax.ShapeDtypeStruct((count, early.shape[1]), jnp.bfloat16),
        in_specs=[spec("scalar")] + [spec()] * (len(tokens) + 2),
        out_specs=spec(),
        scratch_shapes=[pltpu.VMEM((count, model), jnp.bfloat16)],
        compiler_params=limit(16),
    )(places, *tokens, early, late)


def up_kernel(place_ref, *refs, groups, shares):
    last = groups + sum(shares)
    tokens, held = refs[:groups], refs[groups:last]
    units_ref, whole_ref, full_ref = refs[last:]
    joined_rows(held, shares, whole_ref, place_ref)
    joined_columns(tokens, full_ref)
    before = jnp.dot(full_ref[...], whole_ref[...], preferred_element_type=jnp.float32)
    units_ref[...] = jnp.square(jnp.maximum(before, 0.0)).astype(jnp.bfloat16)


def up_whole(places, tokens, held):
    flat, shares = flattened(held)
    rows, width = flat[0].shape[0], sum(part.shape[1] for part in held[0])
    count = sum(x.shape[0] for x in tokens) // 2

    def kernel(*refs):
        up_kernel(*refs, groups=len(tokens), shares=shares)

    return pl.pallas_call(
        kernel,
        out_shape=jax.ShapeDtypeStruct((count, width), jnp.bfloat16),
        in_specs=[spec("scalar")] + [spec()] * (len(tokens) + len(flat)),
        out_specs=spec(),
        scratch_shapes=[
            pltpu.VMEM((rows * len(held), width), jnp.bfloat16),
            pltpu.VMEM((count, rows * len(held)), jnp.bfloat16),
        ],
        compiler_params=limit(32),
    )(places, *tokens, *flat)


def down_kernel(*refs, parts, pieces):
    units = sum(parts)
    hidden, held = refs[:units], refs[units : units + pieces]
    outs, whole_ref = refs[units + pieces : -1], refs[-1]
    cols, count = held[0].shape[1], outs[0].shape[0]
    for i, piece in enumerate(held):
        whole_ref[:, i * cols : (i + 1) * cols] = piece[...]
    at = out = 0
    for part in parts:
        total, begin = None, 0
        for unit in hidden[at : at + part]:
            end = begin + unit.shape[1]
            term = jnp.dot(
                unit[...], whole_ref[begin:end, :], preferred_element_type=jnp.float32
            )
            total, begin = term if total is None else total + term, end
        at += part
        for start in range(0, total.shape[0], count):
            outs[out][...] = total[start : start + count, :].astype(jnp.bfloat16)
            out += 1


def down_project(hidden, held, groups):
    width, cols = held[0].shape
    count = sum(parts[0].shape[0] for parts in hidden) // groups
    out = jax.ShapeDtypeStruct((count, cols * len(held)), jnp.bfloat16)
    flat = [unit for parts in hidden for unit in parts]

    def kernel(*refs):
        down_kernel(*refs, parts=[len(parts) for parts in hidden], pieces=len(held))

    return pl.pallas_call(
        kernel,
        out_shape=[out] * groups,
        in_specs=[spec()] * (len(flat) + len(held)),
        out_specs=[spec()] * groups,
        scratch_shapes=[pltpu.VMEM((width, cols * len(held)), jnp.bfloat16)],
        compiler_params=limit(14),
    )(*flat, *held)


def layer(
    queries, keys, values, documents, sinks, out_weight, residual, norm_gain, up_weight, down_weight
):
    grid = Grid()
    nx, ny, nz, nc = grid.nx, grid.ny, grid.nz, grid.nc
    rows, width = up_weight.shape[0], up_weight.shape[1] // nx

    units = [(dx, i) for dx in range(nx) for i in range(2 if dx and nx == 2 else 1)]
    halo, *up_blocks = prepare(grid, keys, values, documents, up_weight, width, units)
    down_blocks = []
    for u, (dx, i) in enumerate(units):
        if dx:
            up_blocks[u] = grid.send(up_blocks[u], dx=dx)
    for dx in range(nx):
        part = ((grid.x + dx) % nx) * width
        down_part = lax.dynamic_slice(down_weight, (part, 0), (width, rows))
        down_blocks.append(grid.send(down_part, dx=dx) if dx else down_part)

    up_held, up_places = [], []
    for step in range(nz):
        pieces = {(dx, dc): [] for dx in range(nx) for dc in range(nc)}
        for u, (dx, i) in enumerate(units):
            if step:
                up_blocks[u] = grid.send(up_blocks[u], dz=1)
            for dc in range(nc):
                piece = grid.send(up_blocks[u], dc=dc) if dc else up_blocks[u]
                pieces[dx, dc].append(piece)
        for (dx, dc), piece in pieces.items():
            chip = grid.ring_z(step) * nx + (grid.x - dx) % nx
            up_held.append(piece)
            up_places.append(chip * nc + (grid.c - dc) % nc)
    up_places = jnp.stack(up_places)

    down_held = []
    for x in range(nx):
        held = down_blocks[0]
        for dx in range(1, nx):
            held = jnp.where((grid.x - dx) % nx == x, down_blocks[dx], held)
        down_held.append(held)

    pieces = windowed_attention(grid, halo, queries, keys, values, documents, sinks)
    heads = []
    for dy in range(ny):
        heads.append(grid.send(pieces[dy], dy=dy) if dy else pieces[dy])
    places = jnp.stack([(lax.axis_index("tp") - dy) % ny for dy in range(ny)])
    mixed, *normed = project(places, heads, out_weight, residual, norm_gain)

    groups = [(dx, dy) for dx in range(nx) for dy in range(ny)]
    groups.sort(key=lambda group: (group[0] > 0) + (group[1] > 0))
    tokens = {(0, 0): normed}
    for dx, dy in groups[1:]:
        if dx and dy and nx == ny == 2 and rows % 128 == 0:
            left = grid.send(tokens[0, 1][0], dx=1)
            right = grid.send(tokens[1, 0][1], dy=1)
            tokens[dx, dy] = [left, right]
            continue
        tokens[dx, dy] = []
        for half in normed:
            tokens[dx, dy].append(grid.send(half, dx=dx, dy=dy))
    tokens = [tokens[group] for group in groups]
    near = sum(1 for dx, dy in groups if not (dx and dy))
    near_tokens = [half for part in tokens[:near] for half in part]
    if rows % 128 == 0 and near == len(groups) - 1:
        first = (nz - 2) * nx * nc
        *before, early, columns = up_early(up_places, near_tokens, up_held[:first])
        *units, late = up_late(columns, up_held[first:], before)
        hidden = [units, [up_far(up_places, tokens[-1], early, late, rows)]]
    else:
        hidden = [[up_whole(up_places, near_tokens, up_held)]]
        if near < len(groups):
            far_tokens = [half for part in tokens[near:] for half in part]
            hidden.append([up_whole(up_places, far_tokens, up_held)])

    every, per = list(range(nx)), max(1, nz // 4)
    chunks = [(list(range(s, s + per)), every) for s in range(0, nz, per)]
    if nx == 2:
        chunks[-2:] = [(steps, [x]) for steps, _ in chunks[-2:] for x in every]
    columns = {}
    for step in range(nz):
        for x in range(nx):
            if step:
                down_held[x] = grid.send(down_held[x], dz=1)
            for dc in range(nc):
                columns[step, x, dc] = grid.send(down_held[x], dc=dc) if dc else down_held[x]
    out = mixed
    for steps, span in chunks:
        held = [columns[step, x, dc] for step in steps for x in span for dc in range(nc)]
        partial = down_project(hidden, held, len(groups))
        terms = []
        for (dx, dy), piece in zip(groups, partial):
            terms.append(grid.send(piece, dx=-dx, dy=-dy) if dx or dy else piece)
        branch = rounded(sum(term.astype(jnp.float32) for term in terms)).astype(jnp.float32)
        blocks = jnp.split(branch, len(held), axis=1)
        ordered = []
        for i in range(0, len(blocks), nc):
            for c in range(nc):
                block = blocks[i]
                for dc in range(1, nc):
                    block = jnp.where((grid.c - dc) % nc == c, blocks[i + dc], block)
                ordered.append(block)
        each = len(span) * nc
        for i, step in enumerate(steps):
            part = jnp.concatenate(ordered[i * each : (i + 1) * each], axis=1)
            place = ((grid.ring_z(step) * nx + span[0]) * nc) * rows
            before = lax.dynamic_slice(mixed, (0, place), (mixed.shape[0], part.shape[1]))
            after = (before.astype(jnp.float32) + part).astype(jnp.bfloat16)
            out = lax.dynamic_update_slice(out, after, (0, place))
    return out


def solution(mesh):
    in_specs = (
        P("sp", "tp"),
        P("sp", "tp"),
        P("sp", "tp"),
        P("sp"),
        P("tp"),
        P(),
        P(("sp", "tp"), None),
        P(),
        P("sp", "tp"),
        P("tp", "sp"),
    )
    out_specs = P(("sp", "tp"), None)
    return jax.shard_map(layer, mesh=mesh, in_specs=in_specs, out_specs=out_specs, check_vma=False)
```

```python
import functools
import math

import jax
import jax.numpy as jnp
from jax import lax
from jax.experimental import pallas as pl
from jax.experimental.pallas import tpu as pltpu
from jax.sharding import PartitionSpec as P


HEAD_SIZE = 64
WINDOW_REACH = 128


masked_score = -1e30
epsilon = 1e-06
MIB = 1 << 20


class Grid:
    def __init__(self):
        peers, self.ny = lax.axis_size("sp"), lax.axis_size("tp")
        self.nc = 2
        chips = peers // self.nc
        self.nx = math.isqrt(chips // 2)
        self.nz = chips // self.nx
        self.ring = [2 * p if 2 * p < self.nz else 2 * (self.nz - 1 - p) + 1 for p in range(self.nz)]
        sp = lax.axis_index("sp")
        self.c = sp % self.nc
        self.x = (sp // self.nc) % self.nx
        self.z = sp // (self.nc * self.nx)
        self.pos = jnp.where(self.z % 2 == 0, self.z // 2, self.nz - 1 - self.z // 2)

    def send(self, value, dz=0, dx=0, dc=0, dy=0):
        pairs = []
        for p in range(self.nz):
            for x in range(self.nx):
                for c in range(self.nc):
                    for y in range(self.ny):
                        pairs.append(
                            (
                                self.line(self.ring[p], x, c, y),
                                self.line(
                                    self.ring[(p + dz) % self.nz],
                                    (x + dx) % self.nx,
                                    (c + dc) % self.nc,
                                    (y + dy) % self.ny,
                                ),
                            )
                        )
        return lax.ppermute(value, ("sp", "tp"), pairs)

    def line(self, z, x, c, y):
        return ((z * self.nx + x) * self.nc + c) * self.ny + y

    def ring_z(self, step):
        p = (self.pos - step) % self.nz
        return jnp.where(2 * p < self.nz, 2 * p, 2 * (self.nz - 1 - p) + 1)


def passed_along(shard, axis, by):
    peers = lax.axis_size(axis)
    pairs = [(i, i + by) for i in range(peers) if 0 <= i + by < peers]
    return lax.ppermute(shard, axis, pairs)


def rounded(value):
    return lax.optimization_barrier(value.astype(jnp.bfloat16))


def spec(kind=None):
    return pl.BlockSpec(memory_space=pltpu.SMEM if kind == "scalar" else pltpu.VMEM)


def attention_kernel(turn_ref, sinks_ref, docs_ref, q_ref, k_ref, v_ref, halo_ref, *rest):
    outs, whole_ref = rest[:-1], rest[-1]
    length, kv_width = k_ref.shape
    kv_heads = kv_width // HEAD_SIZE
    group = q_ref.shape[1] // kv_width
    reach = WINDOW_REACH
    key = lax.broadcasted_iota(jnp.int32, (2 * reach, reach), 0)
    query = lax.broadcasted_iota(jnp.int32, (2 * reach, reach), 1)
    distance = reach + query - key
    near = (distance >= 0) & (distance < reach)
    halo_docs = [
        halo_ref[2 * reach + start // kv_width * 16 :, :][:1, :] for start in range(0, reach, kv_width)
    ]
    halo_docs = jnp.concatenate(halo_docs, axis=1).astype(jnp.float32)
    halo_docs = jnp.where(turn_ref[len(outs)] == 0, -1.0, halo_docs)
    docs = docs_ref[...].astype(jnp.float32)
    rows = [jnp.broadcast_to(halo_docs, (reach, reach))]
    rows += [jnp.broadcast_to(docs[n : n + 1, :], (reach, reach)) for n in range(length // reach)]
    columns = [row.T for row in rows]
    for n in range(length // reach):
        here = slice(n * reach, (n + 1) * reach)
        back = slice((n - 1) * reach, n * reach)
        same = jnp.concatenate([columns[n], columns[n + 1]], axis=0) == jnp.concatenate(
            [rows[n + 1]] * 2, axis=0
        )
        hide = jnp.where(near & same, 0.0, masked_score)
        hide = jnp.concatenate([hide] * group, axis=1)
        early_k = k_ref[back, :] if n else halo_ref[:reach, :]
        early_v = v_ref[back, :] if n else halo_ref[reach : 2 * reach, :]
        band_k = jnp.concatenate([early_k, k_ref[here, :]], axis=0)
        band_v = jnp.concatenate([early_v, v_ref[here, :]], axis=0)
        for h in range(kv_heads):
            kv = slice(h * HEAD_SIZE, (h + 1) * HEAD_SIZE)
            heads = [h * group + g for g in range(group)]
            q = jnp.concatenate(
                [q_ref[here, i * HEAD_SIZE : (i + 1) * HEAD_SIZE] for i in heads], axis=0
            )
            scores = lax.dot_general(
                band_k[:, kv], q, (((1,), (1,)), ((), ())), preferred_element_type=jnp.float32
            ) * HEAD_SIZE ** (-0.5)
            scores = jnp.where(hide < 0.0, masked_score, scores)
            sink = jnp.concatenate(
                [jnp.full((1, reach), sinks_ref[i], jnp.float32) for i in heads], axis=1
            )
            top = jnp.maximum(jnp.max(scores, axis=0, keepdims=True), sink)
            exponent = jnp.exp(scores - top)
            total = jnp.exp(sink - top) + jnp.sum(exponent, axis=0, keepdims=True)
            shares = (exponent * (1.0 / total)).astype(jnp.bfloat16)
            attended = lax.dot_general(
                band_v[:, kv], shares, (((0,), (0,)), ((), ())), preferred_element_type=jnp.float32
            )
            for g, i in enumerate(heads):
                whole_ref[here, i * HEAD_SIZE : (i + 1) * HEAD_SIZE] = attended[
                    :, g * reach : (g + 1) * reach
                ].T.astype(jnp.bfloat16)
    count = outs[0].shape[0]
    for dy, out in enumerate(outs):
        out[...] = whole_ref[pl.ds(pl.multiple_of(turn_ref[dy] * count, count), count), :]


def prepare_kernel(turn_ref, docs_ref, k_ref, v_ref, up_ref, halo_ref, *refs, width, units, nx):
    parts, sems = refs[:-1], refs[-1]
    reach, kv_width = WINDOW_REACH, k_ref.shape[1]
    last = k_ref.shape[0] - reach
    copies = []
    for i, (part, (dx, at)) in enumerate(zip(parts, units)):
        start = pl.multiple_of(lax.rem(turn_ref[0] + dx, nx) * width + at * part.shape[1], part.shape[1])
        columns = up_ref.at[:, pl.ds(start, part.shape[1])]
        copies.append(pltpu.make_async_copy(columns, part, sems.at[i]))
    for i, ref in enumerate((k_ref, v_ref)):
        to = halo_ref.at[pl.ds(i * reach, reach), :]
        copies.append(
            pltpu.make_async_copy(ref.at[pl.ds(last, reach), :], to, sems.at[len(parts) + i])
        )
    for copy in copies:
        copy.start()
    docs = docs_ref[docs_ref.shape[0] - 1 :, :].astype(jnp.float32).astype(jnp.bfloat16)
    for start in range(0, reach, kv_width):
        row = docs[:, start : start + kv_width]
        at = 2 * reach + start // kv_width * 16
        halo_ref[at : at + 16, :] = jnp.broadcast_to(row, (16, kv_width))
    for copy in copies:
        copy.wait()


def prepare(grid, keys, values, documents, up_weight, width, units):
    kv_width = keys.shape[1]
    shares = [sum(dx == other for other, _ in units) for dx, _ in units]
    parts = [
        jax.ShapeDtypeStruct((up_weight.shape[0], width // share), up_weight.dtype)
        for share in shares
    ]

    def kernel(*refs):
        prepare_kernel(*refs, width=width, units=units, nx=grid.nx)

    docs_rows = 16 * (WINDOW_REACH // kv_width)
    halo = jax.ShapeDtypeStruct((2 * WINDOW_REACH + docs_rows, kv_width), keys.dtype)
    turn = grid.x.reshape(1)
    far = pl.BlockSpec(memory_space=pltpu.HBM)
    return pl.pallas_call(
        kernel,
        out_shape=[halo] + parts,
        in_specs=[spec("scalar"), spec()] + [far] * 3,
        out_specs=[spec()] * (1 + len(parts)),
        scratch_shapes=[pltpu.SemaphoreType.DMA((len(parts) + 2,))],
        compiler_params=pltpu.CompilerParams(vmem_limit_bytes=60 * MIB),
    )(turn, documents.reshape(-1, WINDOW_REACH), keys, values, up_weight)


def windowed_attention(grid, halo, queries, keys, values, documents, sinks):
    length = queries.shape[0]
    halo = passed_along(halo, "sp", 1)
    turn = [(lax.axis_index("tp") + dy) % grid.ny for dy in range(grid.ny)]
    turn = jnp.stack(turn + [lax.axis_index("sp")])
    piece = jax.ShapeDtypeStruct((length // grid.ny, queries.shape[1]), jnp.bfloat16)
    return pl.pallas_call(
        attention_kernel,
        out_shape=[piece] * grid.ny,
        in_specs=[spec("scalar")] * 2 + [spec()] * 5,
        out_specs=[spec()] * grid.ny,
        scratch_shapes=[pltpu.VMEM(queries.shape, jnp.bfloat16)],
        compiler_params=pltpu.CompilerParams(vmem_limit_bytes=8 * MIB),
    )(turn, sinks, documents.reshape(-1, WINDOW_REACH), queries, keys, values, halo)


def project_kernel(place_ref, *refs):
    pieces = refs[:-6]
    weight_ref, residual_ref, gain_ref, mixed_ref, left_ref, right_ref = refs[-6:]
    width = pieces[0].shape[1]
    total = None
    for i, piece in enumerate(pieces):
        start = pl.multiple_of(place_ref[i] * width, width)
        part = jnp.dot(
            piece[...], weight_ref[pl.ds(start, width), :], preferred_element_type=jnp.float32
        )
        total = part if total is None else total + part
    projected = total.astype(jnp.bfloat16).astype(jnp.float32)
    mixed = (residual_ref[...].astype(jnp.float32) + projected).astype(jnp.bfloat16)
    mixed_ref[...] = mixed
    widened = mixed.astype(jnp.float32)
    scale = lax.rsqrt(jnp.mean(widened * widened, axis=-1, keepdims=True) + epsilon)
    normed = (widened * scale * gain_ref[...]).astype(jnp.bfloat16)
    half = left_ref.shape[1]
    left_ref[...] = normed[:, :half]
    right_ref[...] = normed[:, half:]


def project(places, pieces, out_weight, residual, norm_gain):
    count, model = residual.shape
    rows = jax.ShapeDtypeStruct(residual.shape, jnp.bfloat16)
    half = jax.ShapeDtypeStruct((count, model // 2), jnp.bfloat16)
    return pl.pallas_call(
        project_kernel,
        out_shape=[rows, half, half],
        in_specs=[spec("scalar")] + [spec()] * (len(pieces) + 3),
        out_specs=[spec()] * 3,
        compiler_params=pltpu.CompilerParams(vmem_limit_bytes=16 * MIB),
    )(places, *pieces, out_weight, residual, norm_gain.reshape(1, -1))


def joined_columns(halves, out_ref):
    count, half = halves[0].shape
    for i, x_ref in enumerate(halves):
        at, begin = i // 2 * count, i % 2 * half
        out_ref[at : at + count, begin : begin + half] = x_ref[...]


def chosen_columns(place_ref, places, rows, halves, out_ref):
    count, half = halves[0].shape
    each = half // rows
    for i, place in enumerate(places):

        def copy(side, i=i, place=place):
            start = pl.multiple_of((place_ref[place] - side * each) * rows, rows)
            for g, x_ref in enumerate(halves[side::2]):
                out_ref[g * count : (g + 1) * count, i * rows : (i + 1) * rows] = x_ref[
                    :, pl.ds(start, rows)
                ]

        pl.when(place_ref[place] < each)(functools.partial(copy, 0))
        pl.when(place_ref[place] >= each)(functools.partial(copy, 1))


def joined_rows(held, shares, out_ref, place_ref=None):
    rows, at = held[0].shape[0], 0
    for i, share in enumerate(shares):
        place = i if place_ref is None else place_ref[i]
        start, begin = pl.multiple_of(place * rows, rows), 0
        for piece in held[at : at + share]:
            end = begin + piece.shape[1]
            out_ref[pl.ds(start, rows), begin:end] = piece[...]
            begin = end
        at += share


def flattened(held):
    return [part for piece in held for part in piece], [len(piece) for piece in held]


def up_early_kernel(place_ref, *refs, groups, shares):
    last, pieces = groups + sum(shares), len(shares)
    tokens, held = refs[:groups], refs[groups:last]
    *before_refs, whole_ref, late_ref, columns_ref = refs[last:]
    rows = held[0].shape[0]
    joined_rows(held, shares, whole_ref)
    chosen_columns(place_ref, range(pieces), rows, tokens, columns_ref)
    rest = range(pieces, pieces + late_ref.shape[1] // rows)
    chosen_columns(place_ref, rest, rows, tokens, late_ref)
    step = before_refs[0].shape[1]
    for i, before_ref in enumerate(before_refs):
        before_ref[...] = jnp.dot(
            columns_ref[...],
            whole_ref[:, i * step : (i + 1) * step],
            preferred_element_type=jnp.float32,
        )


def up_late_kernel(columns_ref, *refs, shares, early):
    pieces = sum(shares)
    held, early_refs = refs[:pieces], refs[pieces : pieces + early]
    *units_refs, whole_ref = refs[pieces + early :]
    joined_rows(held, shares, whole_ref)
    step, held_width = early_refs[0].shape[1], units_refs[0].shape[1]
    for i, early_ref in enumerate(early_refs):
        cols = slice(i * step, (i + 1) * step)
        before = early_ref[...] + jnp.dot(
            columns_ref[...], whole_ref[:, cols], preferred_element_type=jnp.float32
        )
        units = jnp.square(jnp.maximum(before, 0.0)).astype(jnp.bfloat16)
        at = i * step % held_width
        units_refs[i * step // held_width][:, at : at + step] = units


def up_far_kernel(place_ref, *refs, rows, pieces):
    tokens = refs[:-4]
    early_ref, late_ref, units_ref, columns_ref = refs[-4:]
    chosen_columns(place_ref, range(pieces), rows, tokens, columns_ref)
    cut, width = early_ref.shape
    step = min(width, 512)
    for start in range(0, width, step):
        cols = slice(start, start + step)
        before = jnp.dot(
            columns_ref[:, :cut], early_ref[:, cols], preferred_element_type=jnp.float32
        )
        before += jnp.dot(
            columns_ref[:, cut:], late_ref[:, cols], preferred_element_type=jnp.float32
        )
        units_ref[:, cols] = jnp.square(jnp.maximum(before, 0.0)).astype(jnp.bfloat16)


def limit(mebibytes):
    return pltpu.CompilerParams(vmem_limit_bytes=mebibytes * MIB)


def up_early(places, tokens, held):
    flat, shares = flattened(held)
    rows, width = flat[0].shape[0], sum(part.shape[1] for part in held[0])
    step = min(width, 512)
    count, model = sum(x.shape[0] for x in tokens) // 2, 2 * tokens[0].shape[1]
    depth = rows * len(held)

    def kernel(*refs):
        up_early_kernel(*refs, groups=len(tokens), shares=shares)

    return pl.pallas_call(
        kernel,
        out_shape=[jax.ShapeDtypeStruct((count, step), jnp.float32)] * (width // step)
        + [jax.ShapeDtypeStruct((depth, width), jnp.bfloat16)]
        + [jax.ShapeDtypeStruct((count, model - depth), jnp.bfloat16)],
        in_specs=[spec("scalar")] + [spec()] * (len(tokens) + len(flat)),
        out_specs=[spec()] * (width // step + 2),
        scratch_shapes=[pltpu.VMEM((count, depth), jnp.bfloat16)],
        compiler_params=limit(30),
    )(places, *tokens, *flat)


def up_late(columns, held, early):
    flat, shares = flattened(held)
    rows, width = flat[0].shape[0], sum(part.shape[1] for part in held[0])
    count = columns.shape[0]
    depth = rows * len(held)
    halves = 4

    def kernel(*refs):
        up_late_kernel(*refs, shares=shares, early=len(early))

    return pl.pallas_call(
        kernel,
        out_shape=[jax.ShapeDtypeStruct((count, width // halves), jnp.bfloat16)] * halves
        + [jax.ShapeDtypeStruct((depth, width), jnp.bfloat16)],
        in_specs=[spec()] * (1 + len(flat) + len(early)),
        out_specs=[spec()] * (halves + 1),
        compiler_params=limit(22),
    )(columns, *flat, *early)


def up_far(places, tokens, early, late, rows):
    count, model = tokens[0].shape[0], early.shape[0] + late.shape[0]

    def kernel(*refs):
        up_far_kernel(*refs, rows=rows, pieces=model // rows)

    return pl.pallas_call(
        kernel,
        out_shape=jax.ShapeDtypeStruct((count, early.shape[1]), jnp.bfloat16),
        in_specs=[spec("scalar")] + [spec()] * (len(tokens) + 2),
        out_specs=spec(),
        scratch_shapes=[pltpu.VMEM((count, model), jnp.bfloat16)],
        compiler_params=limit(16),
    )(places, *tokens, early, late)


def up_kernel(place_ref, *refs, groups, shares):
    last = groups + sum(shares)
    tokens, held = refs[:groups], refs[groups:last]
    units_ref, whole_ref, full_ref = refs[last:]
    joined_rows(held, shares, whole_ref, place_ref)
    joined_columns(tokens, full_ref)
    before = jnp.dot(full_ref[...], whole_ref[...], preferred_element_type=jnp.float32)
    units_ref[...] = jnp.square(jnp.maximum(before, 0.0)).astype(jnp.bfloat16)


def up_whole(places, tokens, held):
    flat, shares = flattened(held)
    rows, width = flat[0].shape[0], sum(part.shape[1] for part in held[0])
    count = sum(x.shape[0] for x in tokens) // 2

    def kernel(*refs):
        up_kernel(*refs, groups=len(tokens), shares=shares)

    return pl.pallas_call(
        kernel,
        out_shape=jax.ShapeDtypeStruct((count, width), jnp.bfloat16),
        in_specs=[spec("scalar")] + [spec()] * (len(tokens) + len(flat)),
        out_specs=spec(),
        scratch_shapes=[
            pltpu.VMEM((rows * len(held), width), jnp.bfloat16),
            pltpu.VMEM((count, rows * len(held)), jnp.bfloat16),
        ],
        compiler_params=limit(32),
    )(places, *tokens, *flat)


def down_kernel(*refs, parts, pieces):
    units = sum(parts)
    hidden, held = refs[:units], refs[units : units + pieces]
    outs, whole_ref = refs[units + pieces : -1], refs[-1]
    cols, count = held[0].shape[1], outs[0].shape[0]
    for i, piece in enumerate(held):
        whole_ref[:, i * cols : (i + 1) * cols] = piece[...]
    at = out = 0
    for part in parts:
        total, begin = None, 0
        for unit in hidden[at : at + part]:
            end = begin + unit.shape[1]
            term = jnp.dot(
                unit[...], whole_ref[begin:end, :], preferred_element_type=jnp.float32
            )
            total, begin = term if total is None else total + term, end
        at += part
        for start in range(0, total.shape[0], count):
            outs[out][...] = total[start : start + count, :].astype(jnp.bfloat16)
            out += 1


def down_project(hidden, held, groups):
    width, cols = held[0].shape
    count = sum(parts[0].shape[0] for parts in hidden) // groups
    out = jax.ShapeDtypeStruct((count, cols * len(held)), jnp.bfloat16)
    flat = [unit for parts in hidden for unit in parts]

    def kernel(*refs):
        down_kernel(*refs, parts=[len(parts) for parts in hidden], pieces=len(held))

    return pl.pallas_call(
        kernel,
        out_shape=[out] * groups,
        in_specs=[spec()] * (len(flat) + len(held)),
        out_specs=[spec()] * groups,
        scratch_shapes=[pltpu.VMEM((width, cols * len(held)), jnp.bfloat16)],
        compiler_params=limit(14),
    )(*flat, *held)


def layer(
    queries, keys, values, documents, sinks, out_weight, residual, norm_gain, up_weight, down_weight
):
    grid = Grid()
    nx, ny, nz, nc = grid.nx, grid.ny, grid.nz, grid.nc
    rows, width = up_weight.shape[0], up_weight.shape[1] // nx

    units = [(dx, i) for dx in range(nx) for i in range(2 if dx and nx == 2 else 1)]
    halo, *up_blocks = prepare(grid, keys, values, documents, up_weight, width, units)
    down_blocks = []
    for u, (dx, i) in enumerate(units):
        if dx:
            up_blocks[u] = grid.send(up_blocks[u], dx=dx)
    for dx in range(nx):
        part = ((grid.x + dx) % nx) * width
        down_part = lax.dynamic_slice(down_weight, (part, 0), (width, rows))
        down_blocks.append(grid.send(down_part, dx=dx) if dx else down_part)

    up_held, up_places = [], []
    for step in range(nz):
        pieces = {(dx, dc): [] for dx in range(nx) for dc in range(nc)}
        for u, (dx, i) in enumerate(units):
            if step:
                up_blocks[u] = grid.send(up_blocks[u], dz=1)
            for dc in range(nc):
                piece = grid.send(up_blocks[u], dc=dc) if dc else up_blocks[u]
                pieces[dx, dc].append(piece)
        for (dx, dc), piece in pieces.items():
            chip = grid.ring_z(step) * nx + (grid.x - dx) % nx
            up_held.append(piece)
            up_places.append(chip * nc + (grid.c - dc) % nc)
    up_places = jnp.stack(up_places)

    down_held = []
    for x in range(nx):
        held = down_blocks[0]
        for dx in range(1, nx):
            held = jnp.where((grid.x - dx) % nx == x, down_blocks[dx], held)
        down_held.append(held)

    pieces = windowed_attention(grid, halo, queries, keys, values, documents, sinks)
    heads = []
    for dy in range(ny):
        heads.append(grid.send(pieces[dy], dy=dy) if dy else pieces[dy])
    places = jnp.stack([(lax.axis_index("tp") - dy) % ny for dy in range(ny)])
    mixed, *normed = project(places, heads, out_weight, residual, norm_gain)

    groups = [(dx, dy) for dx in range(nx) for dy in range(ny)]
    groups.sort(key=lambda group: (group[0] > 0) + (group[1] > 0))
    tokens = {(0, 0): normed}
    for dx, dy in groups[1:]:
        if dx and dy and nx == ny == 2 and rows % 128 == 0:
            left = grid.send(tokens[0, 1][0], dx=1)
            right = grid.send(tokens[1, 0][1], dy=1)
            tokens[dx, dy] = [left, right]
            continue
        tokens[dx, dy] = []
        for half in normed:
            tokens[dx, dy].append(grid.send(half, dx=dx, dy=dy))
    tokens = [tokens[group] for group in groups]
    near = sum(1 for dx, dy in groups if not (dx and dy))
    near_tokens = [half for part in tokens[:near] for half in part]
    if rows % 128 == 0 and near == len(groups) - 1:
        first = (nz - 2) * nx * nc
        *before, early, columns = up_early(up_places, near_tokens, up_held[:first])
        *units, late = up_late(columns, up_held[first:], before)
        hidden = [units, [up_far(up_places, tokens[-1], early, late, rows)]]
    else:
        hidden = [[up_whole(up_places, near_tokens, up_held)]]
        if near < len(groups):
            far_tokens = [half for part in tokens[near:] for half in part]
            hidden.append([up_whole(up_places, far_tokens, up_held)])

    every, per = list(range(nx)), max(1, nz // 4)
    chunks = [(list(range(s, s + per)), every) for s in range(0, nz, per)]
    if nx == 2:
        chunks[-2:] = [(steps, [x]) for steps, _ in chunks[-2:] for x in every]
    columns = {}
    for step in range(nz):
        for x in range(nx):
            if step:
                down_held[x] = grid.send(down_held[x], dz=1)
            for dc in range(nc):
                columns[step, x, dc] = grid.send(down_held[x], dc=dc) if dc else down_held[x]
    out = mixed
    for steps, span in chunks:
        held = [columns[step, x, dc] for step in steps for x in span for dc in range(nc)]
        partial = down_project(hidden, held, len(groups))
        terms = []
        for (dx, dy), piece in zip(groups, partial):
            terms.append(grid.send(piece, dx=-dx, dy=-dy) if dx or dy else piece)
        branch = rounded(sum(term.astype(jnp.float32) for term in terms)).astype(jnp.float32)
        blocks = jnp.split(branch, len(held), axis=1)
        ordered = []
        for i in range(0, len(blocks), nc):
            for c in range(nc):
                block = blocks[i]
                for dc in range(1, nc):
                    block = jnp.where((grid.c - dc) % nc == c, blocks[i + dc], block)
                ordered.append(block)
        each = len(span) * nc
        for i, step in enumerate(steps):
            part = jnp.concatenate(ordered[i * each : (i + 1) * each], axis=1)
            place = ((grid.ring_z(step) * nx + span[0]) * nc) * rows
            before = lax.dynamic_slice(mixed, (0, place), (mixed.shape[0], part.shape[1]))
            after = (before.astype(jnp.float32) + part).astype(jnp.bfloat16)
            out = lax.dynamic_update_slice(out, after, (0, place))
    return out


def solution(mesh):
    in_specs = (
        P("sp", "tp"),
        P("sp", "tp"),
        P("sp", "tp"),
        P("sp"),
        P("tp"),
        P(),
        P(("sp", "tp"), None),
        P(),
        P("sp", "tp"),
        P("tp", "sp"),
    )
    out_specs = P(("sp", "tp"), None)
    return jax.shard_map(layer, mesh=mesh, in_specs=in_specs, out_specs=out_specs, check_vma=False)
```
